32 devices in a mesh: fs: 8 (over z, y), tp: 4 (over x, core).
Axes of the slice: x: 2, y: 2, z: 4, core: 2. Of those that a mesh axis runs over, the one named last changes fastest.
Arguments:
- inputs: bfloat16 [4096, 2048], P(('fs', 'tp')), may hold values from -6 to 6
- w_gate: float32 [2048, 5632], P('fs', 'tp'), may hold values from -0.125 to 0.125
- w_value: float32 [2048, 5632], P('fs', 'tp'), may hold values from -0.125 to 0.125
- gate_scale: float32 [5632], P('tp'), may hold values from 0.5 to 2
- value_scale: float32 [5632], P('tp'), may hold values from 0.5 to 2
- conv_gate: float32 [3, 5632], P(None, 'tp'), may hold values from -3.5 to 3.5
- conv_value: float32 [3, 5632], P(None, 'tp'), may hold values from -3.5 to 3.5
- gate_pre: bfloat16 [4096, 5632], P('fs', 'tp'), may hold values from -6 to 6
- value_pre: bfloat16 [4096, 5632], P('fs', 'tp'), may hold values from -6 to 6
- grad_out: bfloat16 [4096, 5632], P('fs', 'tp'), may hold values from -6 to 6
Outputs:
- grad_inputs: bfloat16 [4096, 2048], P(('fs', 'tp'))
- grad_w_gate: float32 [2048, 5632], P('fs', 'tp')
- grad_w_value: float32 [2048, 5632], P('fs', 'tp')
- grad_gate_scale: float32 [5632], P('tp')
- grad_value_scale: float32 [5632], P('tp')
- grad_conv_gate: float32 [3, 5632], P(None, 'tp')
- grad_conv_value: float32 [3, 5632], P(None, 'tp')
The draws below stay inside these ranges and needn't reach their ends.
All inputs are finite; a program needn't handle non-finite values.
Results may differ from the reference program's by a relative error of at most 0.015.
Values may be sent and summed in bfloat16 or wider, within the bound.
A program may use at most 128 MiB of HBM per device.

```python
import math
import jax
import jax.numpy as jnp

D = 2048
FF = 5632
KW = 3
SEQ = 512
TOKENS = 4096
N_FS = 8
N_TP = 4


def strengthened(result, rng, source, target, parts, factor):
    def block_of(position):
        return (jnp.arange(result.shape[position]) // (result.shape[position] // parts)).reshape((-1,) + (1,) * (result.ndim - 1 - position))

    one_side = jax.random.permutation(rng, parts)[block_of(target)]
    second = (block_of(target) + parts // 2) % parts
    return jnp.where((block_of(source) == one_side) | (block_of(source) == second), factor * result, result)


def levels(key, dims, split, least, largest):
    factor_of = 1.0
    for dim, shards_of in split:
        draws = jax.random.uniform(jax.random.fold_in(jax.random.fold_in(key, 6), dim), (shards_of,), jnp.float32, least / len(split), largest / len(split))
        factor_of = factor_of * jnp.repeat(jnp.exp(draws), dims[dim] // shards_of).reshape((-1,) + (1,) * (len(dims) - 1 - dim))
    return factor_of


def bell_draw(rng, dims, scale, most, shards=(), held_as=jnp.bfloat16):
    result = jax.random.normal(rng, dims, jnp.float32) * scale
    if len(shards) > 0:
        result = levels(rng, dims, shards, -0.22, 0.18) * result
    return jnp.clip(result, min=-most, max=most).astype(held_as)


def gaussian_with(stream_key, extent, spread, reach, shards, heavy, dtype=jnp.bfloat16):
    array = spread * jax.random.normal(stream_key, extent, jnp.float32)
    if shards:
        array = array * levels(stream_key, extent, shards, -0.22, 0.18)
    return jnp.clip(strengthened(array, jax.random.fold_in(stream_key, 3), *heavy), -reach, reach).astype(dtype)


def setup_inputs(seed: int = 0) -> dict:
    key_of = jax.random.split(jax.random.key(seed), 11)
    inputs = gaussian_with(key_of[0], (TOKENS, D), 1.0, 6.0, ((0, 32),), (0, 1, 32, 2.75))
    w_gate = bell_draw(key_of[1], (D, FF), D ** -0.5, 0.125, ((0, 8), (1, 4)), jnp.float32)
    w_value = bell_draw(key_of[2], (D, FF), D ** -0.5, 0.125, ((0, 8), (1, 4)), jnp.float32)
    gate_scale = jnp.clip(jnp.exp(math.log(2.0) - 1.3862944 * jax.random.uniform(key_of[3], (FF,), jnp.float32) ** levels(key_of[3], (FF,), ((0, 4),), -0.2, 0.2)), 0.5, 2.0)
    value_scale = jnp.clip(jnp.exp(math.log(2.0) - 1.3862944 * jax.random.uniform(key_of[4], (FF,), jnp.float32) ** levels(key_of[4], (FF,), ((0, 4),), -0.2, 0.2)), 0.5, 2.0)
    conv_gate = bell_draw(key_of[5], (KW, FF), KW ** -0.5, 3.5, ((1, 4),), jnp.float32)
    conv_value = bell_draw(key_of[6], (KW, FF), KW ** -0.5, 3.5, ((1, 4),), jnp.float32)
    gate_pre = bell_draw(key_of[7], (TOKENS, FF), 1.0, 6.0, ((0, 8), (1, 4)))
    value_pre = bell_draw(key_of[8], (TOKENS, FF), 1.0, 6.0, ((0, 8), (1, 4)))
    grad_out = gaussian_with(key_of[9], (TOKENS, FF), 1.0, 6.0, ((0, 8), (1, 4)), (0, 1, 8, 2.0))
    return {"inputs": inputs, "w_gate": w_gate, "w_value": w_value, "gate_scale": gate_scale, "value_scale": value_scale, "conv_gate": conv_gate, "conv_value": conv_value, "gate_pre": gate_pre, "value_pre": value_pre, "grad_out": grad_out}


def shift_down(field, steps):
    return jnp.pad(field, ((0, 0), (steps, 0), (0, 0)))[:, :field.shape[1]]


def shift_up(field, steps):
    return jnp.pad(field, ((0, 0), (0, steps), (0, 0)))[:, steps:]


def reference(inputs, w_gate, w_value, gate_scale, value_scale, conv_gate, conv_value, gate_pre, value_pre, grad_out):
    gate_raw = gate_pre.astype(jnp.float32).reshape(N_FS, SEQ, FF)
    value_raw = value_pre.astype(jnp.float32).reshape(N_FS, SEQ, FF)
    gate_lin = gate_raw * gate_scale
    value_lin = value_raw * value_scale
    gate_conv = conv_gate[2] * gate_lin + conv_gate[1] * shift_down(gate_lin, 1) + conv_gate[0] * shift_down(gate_lin, 2)
    value_conv = conv_value[2] * value_lin + conv_value[1] * shift_down(value_lin, 1) + conv_value[0] * shift_down(value_lin, 2)
    sig = jax.nn.sigmoid(gate_conv)
    upstream = grad_out.astype(jnp.float32).reshape(N_FS, SEQ, FF)
    d_gate_conv = upstream * value_conv * sig * (1.0 + gate_conv * (1.0 - sig))
    d_value_conv = upstream * gate_conv * sig
    grad_conv_gate = jnp.stack([jnp.sum(d_gate_conv * shift_down(gate_lin, 2), axis=(0, 1)),
                                jnp.sum(d_gate_conv * shift_down(gate_lin, 1), axis=(0, 1)),
                                jnp.sum(d_gate_conv * gate_lin, axis=(0, 1))])
    grad_conv_value = jnp.stack([jnp.sum(d_value_conv * shift_down(value_lin, 2), axis=(0, 1)),
                                 jnp.sum(d_value_conv * shift_down(value_lin, 1), axis=(0, 1)),
                                 jnp.sum(d_value_conv * value_lin, axis=(0, 1))])
    d_gate_lin = conv_gate[2] * d_gate_conv + conv_gate[1] * shift_up(d_gate_conv, 1) + conv_gate[0] * shift_up(d_gate_conv, 2)
    d_value_lin = conv_value[2] * d_value_conv + conv_value[1] * shift_up(d_value_conv, 1) + conv_value[0] * shift_up(d_value_conv, 2)
    grad_gate_scale = jnp.sum(d_gate_lin * gate_raw, axis=(0, 1))
    grad_value_scale = jnp.sum(d_value_lin * value_raw, axis=(0, 1))
    d_gate_lin = d_gate_lin.reshape(TOKENS, FF)
    d_value_lin = d_value_lin.reshape(TOKENS, FF)
    gate_cot = d_gate_lin.astype(jnp.bfloat16)
    value_cot = d_value_lin.astype(jnp.bfloat16)
    gate_back = (d_gate_lin * gate_scale).astype(jnp.bfloat16)
    value_back = (d_value_lin * value_scale).astype(jnp.bfloat16)
    grad_w_gate = jnp.dot(inputs.T, gate_cot, preferred_element_type=jnp.float32) * gate_scale
    grad_w_value = jnp.dot(inputs.T, value_cot, preferred_element_type=jnp.float32) * value_scale
    gate_half = w_gate.astype(jnp.bfloat16)
    value_half = w_value.astype(jnp.bfloat16)
    width = FF // N_TP
    total = jnp.zeros((TOKENS, D), jnp.float32)
    for block in range(N_TP):
        lo = block * width
        part = jnp.dot(gate_back[:, lo:lo + width], gate_half[:, lo:lo + width].T, preferred_element_type=jnp.float32)
        part = part + jnp.dot(value_back[:, lo:lo + width], value_half[:, lo:lo + width].T, preferred_element_type=jnp.float32)
        total = total + part.astype(jnp.bfloat16).astype(jnp.float32)
    grad_inputs = total.astype(jnp.bfloat16)
    return (grad_inputs, grad_w_gate, grad_w_value, grad_gate_scale, grad_value_scale, grad_conv_gate, grad_conv_value)
```

```python
import jax
import jax.numpy as jnp
from jax import lax
from jax.sharding import PartitionSpec as P


BF = jnp.bfloat16
F32 = jnp.float32


def shift_down(field, steps):
    return jnp.pad(field, ((steps, 0), (0, 0)))[: field.shape[0]]


def shift_up(field, steps):
    return jnp.pad(field, ((0, steps), (0, 0)))[steps:]


def tdot(a, b):
    return lax.dot_general(a, b, (((0,), (0,)), ((), ())), preferred_element_type=F32)


def ndot(a, b):
    return lax.dot_general(a, b, (((1,), (1,)), ((), ())), preferred_element_type=F32)


def make(n_fs, n_tp):
    links = n_fs // 2

    def on_device(
        inputs,
        w_gate,
        w_value,
        gate_scale,
        value_scale,
        conv_gate,
        conv_value,
        gate_pre,
        value_pre,
        grad_out,
    ):
        fs = lax.axis_index("fs")
        tp = lax.axis_index("tp")
        c, y = fs // 2, fs % 2
        rows, depth = inputs.shape
        own = w_gate.shape[0]
        half = depth // 2
        tokens, columns = gate_pre.shape

        def swap(x, axis, bit, n):
            return lax.ppermute(x, axis, [(i, i ^ bit) for i in range(n)])

        def chain(x, right, senders):
            step = 1 if right else -1
            pairs = [(2 * s + j, 2 * (s + step) + j) for s in senders for j in (0, 1)]
            return lax.ppermute(x, "fs", pairs)

        def spread(block):
            rights, lefts = [], []
            r = l = block
            for s in range(links - 1):
                r = chain(r, True, range(s, links - 1))
                l = chain(l, False, range(1, links - s))
                rights.append(r)
                lefts.append(l)
            return rights, lefts

        weights = [
            spread((w * scale).astype(BF))
            for w, scale in ((w_gate, gate_scale), (w_value, value_scale))
        ]

        by_half = inputs.reshape(rows, links, 2, own)
        mine = lax.dynamic_index_in_dim(by_half, y, 2, keepdims=False)
        other = lax.dynamic_index_in_dim(by_half, 1 - y, 2, keepdims=False)
        mine, other = mine.reshape(rows, half), other.reshape(rows, half)
        x = jnp.stack([mine, swap(other, "fs", 1, n_fs)])[:, None]
        bit = n_tp // 2
        while bit:
            got = swap(x, "tp", bit, n_tp)
            high = (tp // bit) % 2 == 1
            x = jnp.where(high, jnp.stack([got, x], 2), jnp.stack([x, got], 2))
            x = x.reshape(2, -1, rows, half)
            bit //= 2
        x = x.reshape(2, tokens, half)

        gate_raw = gate_pre.astype(F32)
        value_raw = value_pre.astype(F32)
        gate_lin = gate_raw * gate_scale
        value_lin = value_raw * value_scale
        gate_conv = (
            conv_gate[2] * gate_lin
            + conv_gate[1] * shift_down(gate_lin, 1)
            + conv_gate[0] * shift_down(gate_lin, 2)
        )
        value_conv = (
            conv_value[2] * value_lin
            + conv_value[1] * shift_down(value_lin, 1)
            + conv_value[0] * shift_down(value_lin, 2)
        )
        sig = jax.nn.sigmoid(gate_conv)
        upstream = grad_out.astype(F32)
        d_gate_conv = upstream * value_conv * sig * (1.0 + gate_conv * (1.0 - sig))
        d_value_conv = upstream * gate_conv * sig

        def back(d, taps):
            return taps[2] * d + taps[1] * shift_up(d, 1) + taps[0] * shift_up(d, 2)

        def tap_sums(d, lin):
            return [jnp.sum(d * shift_down(lin, 2 - j), axis=0) for j in range(3)]

        d_gate_lin = back(d_gate_conv, conv_gate)
        d_value_lin = back(d_value_conv, conv_value)
        sums = jnp.stack(
            [jnp.sum(d_gate_lin * gate_raw, axis=0)]
            + [jnp.sum(d_value_lin * value_raw, axis=0)]
            + tap_sums(d_gate_conv, gate_lin)
            + tap_sums(d_value_conv, value_lin)
        )
        bit = 1
        while bit < n_fs:
            sums = sums + swap(sums, "fs", bit, n_fs)
            bit *= 2

        cots = [d_gate_lin.astype(BF), d_value_lin.astype(BF)]
        pair = [(cot, swap(cot, "fs", 1, n_fs)) for cot in cots]

        def at(blocks, i):
            return lax.dynamic_index_in_dim(
                blocks, jnp.clip(i, 0, links - 1), 0, keepdims=False
            )

        def collect(parts):
            r = l = None
            for t in range(links - 1):
                send_r = at(parts, links - 1 - t + c)
                send_l = at(parts, c - (links - 1 - t) + 0)
                if t:
                    send_r = (send_r.astype(F32) + r.astype(F32)).astype(BF)
                    send_l = (send_l.astype(F32) + l.astype(F32)).astype(BF)
                r = chain(send_r, True, range(0, t + 1))
                l = chain(send_l, False, range(links - 1 - t, links))
            total = at(parts, c).astype(F32)
            if r is not None:
                total = total + r.astype(F32) + l.astype(F32)
            return total

        grads = []
        for (cot, theirs), scale in zip(pair, (gate_scale, value_scale)):
            parts = (tdot(x[0], cot) + tdot(x[1], theirs)).astype(BF)
            grads.append(collect(parts.reshape(links, own, columns)) * scale)

        whole = []
        for w, scale, (rights, lefts) in zip(
            (w_gate, w_value), (gate_scale, value_scale), weights
        ):
            blocks = [(w * scale).astype(BF)]
            for s in range(links - 1):
                blocks.append(jnp.where(c > s, rights[s], lefts[links - 2 - s]))
            whole.append(jnp.concatenate(blocks, 0))
        part = jnp.stack(
            [
                (ndot(g, whole[0]) + ndot(v, whole[1])).astype(BF)
                for g, v in zip(pair[0], pair[1])
            ]
        ).reshape(2, n_tp, rows, half)
        bit = 1
        while bit < n_tp:
            split = part.reshape(2, -1, 2, rows, half)
            which = (tp // bit) % 2
            keep = lax.dynamic_index_in_dim(split, which, 2, keepdims=False)
            send = lax.dynamic_index_in_dim(split, 1 - which, 2, keepdims=False)
            got = swap(send, "tp", bit, n_tp)
            part = (keep.astype(F32) + got.astype(F32)).astype(BF)
            bit *= 2
        mine = part.reshape(2, rows, half)[0]
        other = swap(part.reshape(2, rows, half)[1], "fs", 1, n_fs)
        both = jnp.where(
            y == 0, jnp.stack([mine, other], 1), jnp.stack([other, mine], 1)
        ).reshape(rows, 2, links, own)
        order = (c - jnp.arange(links)) % links
        grad_inputs = jnp.take(both, order, axis=2).transpose(0, 2, 1, 3)
        return (
            grad_inputs.reshape(rows, depth),
            grads[0],
            grads[1],
            sums[0],
            sums[1],
            sums[2:5],
            sums[5:8],
        )

    return on_device


def solution(mesh):
    placed = (
        P(("fs", "tp"), None),
        P("fs", "tp"),
        P("fs", "tp"),
        P("tp"),
        P("tp"),
        P(None, "tp"),
        P(None, "tp"),
        P("fs", "tp"),
        P("fs", "tp"),
        P("fs", "tp"),
    )
    return jax.shard_map(
        make(mesh.shape["fs"], mesh.shape["tp"]),
        mesh=mesh,
        in_specs=placed,
        out_specs=(
            P(("fs", "tp"), None),
            P("fs", "tp"),
            P("fs", "tp"),
            P("tp"),
            P("tp"),
            P(None, "tp"),
            P(None, "tp"),
        ),
        check_vma=False,
    )
```

```python
import jax
import jax.numpy as jnp
from jax import lax
from jax.experimental import pallas as pl
from jax.experimental.pallas import tpu as pltpu
from jax.sharding import PartitionSpec as P


BF = jnp.bfloat16
F32 = jnp.float32


LANES = 128


def elementwise(gs_ref, vs_ref, cg_ref, cv_ref, g_ref, v_ref, up_ref, gc_ref, vc_ref, s_ref):
    tokens = g_ref.shape[0]
    row = lax.broadcasted_iota(jnp.int32, g_ref.shape, 0)

    def down(x, k):
        return jnp.where(row >= k, pltpu.roll(x, k, 0), 0.0)

    def up(x, k):
        return jnp.where(row < tokens - k, pltpu.roll(x, tokens - k, 0), 0.0)

    def shifted(ref):
        x = ref[...].astype(F32)
        return down(x, 2), down(x, 1), x

    def conv(taps, xs):
        return taps[0:1] * xs[0] + taps[1:2] * xs[1] + taps[2:3] * xs[2]

    def back(taps, d):
        return (taps[2:3] * d + taps[1:2] * up(d, 1) + taps[0:1] * up(d, 2)).astype(BF)

    gs, vs = shifted(g_ref), shifted(v_ref)
    g = conv(cg_ref[...] * gs_ref[...], gs)
    v = conv(cv_ref[...] * vs_ref[...], vs)
    sig = 1.0 / (1.0 + jnp.exp(-g))
    base = up_ref[...].astype(F32) * sig
    d_gate = base * v * (1.0 + g * (1.0 - sig))
    d_value = base * g
    for j in range(3):
        s_ref[j : j + 1] = jnp.sum(d_gate * gs[j], axis=0, keepdims=True)
        s_ref[3 + j : 4 + j] = jnp.sum(d_value * vs[j], axis=0, keepdims=True)
    s_ref[6:8] = jnp.zeros((2, g_ref.shape[1]), F32)
    gc_ref[...] = back(cg_ref[...], d_gate)
    vc_ref[...] = back(cv_ref[...], d_value)


def cotangents(gs, vs, cg, cv, g, v, up):
    tokens, columns = g.shape
    big = pl.BlockSpec((tokens, LANES), lambda i: (0, i))

    def small(n):
        return pl.BlockSpec((n, LANES), lambda i: (0, i))

    return pl.pallas_call(
        elementwise,
        grid=(pl.cdiv(columns, LANES),),
        in_specs=[small(1), small(1), small(3), small(3), big, big, big],
        out_specs=[big, big, small(8)],
        out_shape=[jax.ShapeDtypeStruct(g.shape, BF)] * 2
        + [jax.ShapeDtypeStruct((8, columns), F32)],
        compiler_params=pltpu.CompilerParams(vmem_limit_bytes=24 * 2**20),
        cost_estimate=pl.CostEstimate(
            flops=g.size * 400, bytes_accessed=g.size * 10, transcendentals=g.size
        ),
    )(gs[None], vs[None], cg, cv, g, v, up)


def rescale(gs_ref, vs_ref, g_ref, v_ref, out_ref):
    out_ref[0] = (g_ref[...] * gs_ref[...]).astype(BF)
    out_ref[1] = (v_ref[...] * vs_ref[...]).astype(BF)


def scaled_weights(gs, vs, g, v):
    own, columns = g.shape
    parts = 4
    block = pl.BlockSpec((own // parts, columns), lambda i: (i, 0))
    scale = pl.BlockSpec((1, columns), lambda i: (0, 0))
    return pl.pallas_call(
        rescale,
        grid=(parts,),
        in_specs=[scale, scale, block, block],
        out_specs=pl.BlockSpec((2, own // parts, columns), lambda i: (0, i, 0)),
        out_shape=jax.ShapeDtypeStruct((2, own, columns), BF),
        compiler_params=pltpu.CompilerParams(vmem_limit_bytes=24 * 2**20),
        cost_estimate=pl.CostEstimate(
            flops=g.size * 100, bytes_accessed=g.size * 12, transcendentals=0
        ),
    )(gs[None], vs[None], g, v)


def tdot(a, b):
    return lax.dot_general(a, b, (((0,), (0,)), ((), ())), preferred_element_type=F32)


def ndot(a, b):
    return lax.dot_general(a, b, (((1,), (1,)), ((), ())), preferred_element_type=F32)


def make(n_fs, n_tp):
    links = n_fs // 2

    def on_device(
        inputs,
        w_gate,
        w_value,
        gate_scale,
        value_scale,
        conv_gate,
        conv_value,
        gate_pre,
        value_pre,
        grad_out,
    ):
        fs = lax.axis_index("fs")
        tp = lax.axis_index("tp")
        c, y = fs // 2, fs % 2
        rows, depth = inputs.shape
        own = w_gate.shape[0]
        half = depth // 2
        tokens, columns = gate_pre.shape

        def swap(x, axis, bit, n):
            return lax.ppermute(x, axis, [(i, i ^ bit) for i in range(n)])

        def chain(x, right, senders):
            step = 1 if right else -1
            pairs = [(2 * s + j, 2 * (s + step) + j) for s in senders for j in (0, 1)]
            return lax.ppermute(x, "fs", pairs)

        stacked = scaled_weights(gate_scale, value_scale, w_gate, w_value)
        rights, lefts = [], []
        r = l = stacked
        for s in range(links - 1):
            r = chain(r, True, range(s, links - 1))
            l = chain(l, False, range(1, links - s))
            rights.append(r)
            lefts.append(l)

        by_half = inputs.reshape(rows, links, 2, own)
        mine = lax.dynamic_index_in_dim(by_half, y, 2, keepdims=False)
        other = lax.dynamic_index_in_dim(by_half, 1 - y, 2, keepdims=False)
        mine, other = mine.reshape(rows, half), other.reshape(rows, half)
        other = swap(other, "fs", 1, n_fs)
        x = jnp.stack([mine, other])[:, None]
        bit = n_tp // 2
        while bit:
            got = swap(x, "tp", bit, n_tp)
            high = (tp // bit) % 2 == 1
            x = jnp.where(high, jnp.stack([got, x], 2), jnp.stack([x, got], 2))
            x = x.reshape(2, -1, rows, half)
            bit //= 2
        x = x.reshape(2, tokens, half)

        gate_cot, value_cot, sums = cotangents(
            gate_scale, value_scale, conv_gate, conv_value, gate_pre, value_pre, grad_out
        )
        bit = 1
        while bit < n_fs:
            sums = sums + swap(sums, "fs", bit, n_fs)
            bit *= 2

        gate_theirs = swap(gate_cot, "fs", 1, n_fs)
        value_theirs = swap(value_cot, "fs", 1, n_fs)
        pair = [(gate_cot, gate_theirs), (value_cot, value_theirs)]

        def at(blocks, i):
            return lax.dynamic_index_in_dim(
                blocks, jnp.clip(i, 0, links - 1), 0, keepdims=False
            )

        def collect(parts):
            r = l = None
            for t in range(links - 1):
                send_r = at(parts, links - 1 - t + c)
                send_l = at(parts, c - (links - 1 - t) + 0)
                if t:
                    send_r = (send_r.astype(F32) + r.astype(F32)).astype(BF)
                    send_l = (send_l.astype(F32) + l.astype(F32)).astype(BF)
                r = chain(send_r, True, range(0, t + 1))
                l = chain(send_l, False, range(links - 1 - t, links))
            total = at(parts, c).astype(F32)
            if r is not None:
                total = total + r.astype(F32) + l.astype(F32)
            return total

        grads = []
        for (cot, theirs), scale in zip(pair, (gate_scale, value_scale)):
            first = tdot(x[0], cot)
            parts = (first + tdot(x[1], theirs)).astype(BF)
            blocks = parts.reshape(links, own, columns)
            grads.append(collect(blocks) * scale)

        blocks = [stacked]
        for s in range(links - 1):
            blocks.append(jnp.where(c > s, rights[s], lefts[links - 2 - s]))
        whole = jnp.concatenate(blocks, 1)
        part = jnp.stack(
            [
                (ndot(g, whole[0]) + ndot(v, whole[1])).astype(BF)
                for g, v in zip(pair[0], pair[1])
            ]
        )
        part = part.reshape(2, n_tp, rows, half)
        bit = 1
        while bit < n_tp:
            split = part.reshape(2, -1, 2, rows, half)
            which = (tp // bit) % 2
            keep = lax.dynamic_index_in_dim(split, which, 2, keepdims=False)
            send = lax.dynamic_index_in_dim(split, 1 - which, 2, keepdims=False)
            got = swap(send, "tp", bit, n_tp)
            part = (keep.astype(F32) + got.astype(F32)).astype(BF)
            bit *= 2
        mine = part.reshape(2, rows, half)[0]
        other = swap(part.reshape(2, rows, half)[1], "fs", 1, n_fs)
        both = jnp.where(
            y == 0, jnp.stack([mine, other], 1), jnp.stack([other, mine], 1)
        ).reshape(rows, 2, links, own)
        order = (c - jnp.arange(links)) % links
        grad_inputs = jnp.take(both, order, axis=2).transpose(0, 2, 1, 3)
        return (
            grad_inputs.reshape(rows, depth),
            grads[0],
            grads[1],
            jnp.sum(conv_gate * sums[0:3], axis=0),
            jnp.sum(conv_value * sums[3:6], axis=0),
            sums[0:3] * gate_scale,
            sums[3:6] * value_scale,
        )

    return on_device


def solution(mesh):
    placed = (
        P(("fs", "tp"), None),
        P("fs", "tp"),
        P("fs", "tp"),
        P("tp"),
        P("tp"),
        P(None, "tp"),
        P(None, "tp"),
        P("fs", "tp"),
        P("fs", "tp"),
        P("fs", "tp"),
    )
    body = make(mesh.shape["fs"], mesh.shape["tp"])

    return jax.shard_map(
        body,
        mesh=mesh,
        in_specs=placed,
        out_specs=(
            P(("fs", "tp"), None),
            P("fs", "tp"),
            P("fs", "tp"),
            P("tp"),
            P("tp"),
            P(None, "tp"),
            P(None, "tp"),
        ),
        check_vma=False,
    )
```

```python
import jax
import jax.numpy as jnp
from jax import lax
from jax.experimental import pallas as pl
from jax.experimental.pallas import tpu as pltpu
from jax.sharding import PartitionSpec as P


BF = jnp.bfloat16
F32 = jnp.float32


LANES = 128


def elementwise(gs_ref, vs_ref, cg_ref, cv_ref, g_ref, v_ref, up_ref, gc_ref, vc_ref, s_ref):
    tokens = g_ref.shape[0]
    row = lax.broadcasted_iota(jnp.int32, g_ref.shape, 0)

    def down(x, k):
        return jnp.where(row >= k, pltpu.roll(x, k, 0), 0.0)

    def up(x, k):
        return jnp.where(row < tokens - k, pltpu.roll(x, tokens - k, 0), 0.0)

    def shifted(ref):
        x = ref[...].astype(F32)
        return down(x, 2), down(x, 1), x

    def conv(taps, xs):
        return taps[0:1] * xs[0] + taps[1:2] * xs[1] + taps[2:3] * xs[2]

    def back(taps, d):
        return (taps[2:3] * d + taps[1:2] * up(d, 1) + taps[0:1] * up(d, 2)).astype(BF)

    gs, vs = shifted(g_ref), shifted(v_ref)
    g = conv(cg_ref[...] * gs_ref[...], gs)
    v = conv(cv_ref[...] * vs_ref[...], vs)
    sig = 1.0 / (1.0 + jnp.exp(-g))
    base = up_ref[...].astype(F32) * sig
    d_gate = base * v * (1.0 + g * (1.0 - sig))
    d_value = base * g
    for j in range(3):
        s_ref[j : j + 1] = jnp.sum(d_gate * gs[j], axis=0, keepdims=True)
        s_ref[3 + j : 4 + j] = jnp.sum(d_value * vs[j], axis=0, keepdims=True)
    s_ref[6:8] = jnp.zeros((2, g_ref.shape[1]), F32)
    gc_ref[...] = back(cg_ref[...], d_gate)
    vc_ref[...] = back(cv_ref[...], d_value)


def cotangents(gs, vs, cg, cv, g, v, up):
    tokens, columns = g.shape
    big = pl.BlockSpec((tokens, LANES), lambda i: (0, i))

    def small(n):
        return pl.BlockSpec((n, LANES), lambda i: (0, i))

    return pl.pallas_call(
        elementwise,
        grid=(pl.cdiv(columns, LANES),),
        in_specs=[small(1), small(1), small(3), small(3), big, big, big],
        out_specs=[big, big, small(8)],
        out_shape=[jax.ShapeDtypeStruct(g.shape, BF)] * 2
        + [jax.ShapeDtypeStruct((8, columns), F32)],
        compiler_params=pltpu.CompilerParams(vmem_limit_bytes=24 * 2**20),
        cost_estimate=pl.CostEstimate(
            flops=g.size * 400, bytes_accessed=g.size * 10, transcendentals=g.size
        ),
    )(gs[None], vs[None], cg, cv, g, v, up)


def rescale(gs_ref, vs_ref, g_ref, v_ref, out_ref):
    out_ref[0] = (g_ref[...] * gs_ref[...]).astype(BF)
    out_ref[1] = (v_ref[...] * vs_ref[...]).astype(BF)


def scaled_weights(gs, vs, g, v):
    own, columns = g.shape
    parts = 4
    block = pl.BlockSpec((own // parts, columns), lambda i: (i, 0))
    scale = pl.BlockSpec((1, columns), lambda i: (0, 0))
    return pl.pallas_call(
        rescale,
        grid=(parts,),
        in_specs=[scale, scale, block, block],
        out_specs=pl.BlockSpec((2, own // parts, columns), lambda i: (0, i, 0)),
        out_shape=jax.ShapeDtypeStruct((2, own, columns), BF),
        compiler_params=pltpu.CompilerParams(vmem_limit_bytes=24 * 2**20),
        cost_estimate=pl.CostEstimate(
            flops=g.size * 100, bytes_accessed=g.size * 12, transcendentals=0
        ),
    )(gs[None], vs[None], g, v)


def tdot(a, b):
    return lax.dot_general(a, b, (((0,), (0,)), ((), ())), preferred_element_type=F32)


def ndot(a, b):
    return lax.dot_general(a, b, (((1,), (1,)), ((), ())), preferred_element_type=F32)


def make(n_fs, n_tp):
    links = n_fs // 2

    def on_device(
        inputs,
        w_gate,
        w_value,
        gate_scale,
        value_scale,
        conv_gate,
        conv_value,
        gate_pre,
        value_pre,
        grad_out,
    ):
        fs = lax.axis_index("fs")
        tp = lax.axis_index("tp")
        c, y = fs // 2, fs % 2
        rows, depth = inputs.shape
        own = w_gate.shape[0]
        half = depth // 2
        tokens, columns = gate_pre.shape

        def swap(x, axis, bit, n):
            return lax.ppermute(x, axis, [(i, i ^ bit) for i in range(n)])

        def chain(x, right, senders):
            step = 1 if right else -1
            pairs = [(2 * s + j, 2 * (s + step) + j) for s in senders for j in (0, 1)]
            return lax.ppermute(x, "fs", pairs)

        stacked = scaled_weights(gate_scale, value_scale, w_gate, w_value)
        rights, lefts = [], []
        r = l = stacked
        for s in range(links - 1):
            r = chain(r, True, range(s, links - 1))
            l = chain(l, False, range(1, links - s))
            rights.append(r)
            lefts.append(l)

        by_half = inputs.reshape(rows, links, 2, own)
        mine = lax.dynamic_index_in_dim(by_half, y, 2, keepdims=False)
        other = lax.dynamic_index_in_dim(by_half, 1 - y, 2, keepdims=False)
        mine, other = mine.reshape(rows, half), other.reshape(rows, half)
        other = swap(other, "fs", 1, n_fs)
        x = jnp.stack([mine, other])[:, None]
        bit = n_tp // 2
        while bit:
            got = swap(x, "tp", bit, n_tp)
            high = (tp // bit) % 2 == 1
            x = jnp.where(high, jnp.stack([got, x], 2), jnp.stack([x, got], 2))
            x = x.reshape(2, -1, rows, half)
            bit //= 2
        x = x.reshape(2, tokens, half)

        gate_cot, value_cot, sums = cotangents(
            gate_scale, value_scale, conv_gate, conv_value, gate_pre, value_pre, grad_out
        )
        bit = 1
        while bit < n_fs:
            sums = sums + swap(sums, "fs", bit, n_fs)
            bit *= 2

        gate_theirs = swap(gate_cot, "fs", 1, n_fs)
        value_theirs = swap(value_cot, "fs", 1, n_fs)
        pair = [(gate_cot, gate_theirs), (value_cot, value_theirs)]

        def at(blocks, i):
            return lax.dynamic_index_in_dim(
                blocks, jnp.clip(i, 0, links - 1), 0, keepdims=False
            )

        def collect(parts):
            r = l = None
            for t in range(links - 1):
                send_r = at(parts, links - 1 - t + c)
                send_l = at(parts, c - (links - 1 - t) + 0)
                if t:
                    send_r = (send_r.astype(F32) + r.astype(F32)).astype(BF)
                    send_l = (send_l.astype(F32) + l.astype(F32)).astype(BF)
                r = chain(send_r, True, range(0, t + 1))
                l = chain(send_l, False, range(links - 1 - t, links))
            total = at(parts, c).astype(F32)
            if r is not None:
                total = total + r.astype(F32) + l.astype(F32)
            return total

        grads = []
        for (cot, theirs), scale in zip(pair, (gate_scale, value_scale)):
            first = tdot(x[0], cot)
            parts = (first + tdot(x[1], theirs)).astype(BF)
            blocks = parts.reshape(links, own, columns)
            grads.append(collect(blocks) * scale)

        blocks = [stacked]
        for s in range(links - 1):
            blocks.append(jnp.where(c > s, rights[s], lefts[links - 2 - s]))
        columns_of = []
        for block in blocks:
            columns_of.append(
                [
                    (ndot(g, block[0]) + ndot(v, block[1])).astype(BF)
                    for g, v in zip(pair[0], pair[1])
                ]
            )
        part = jnp.stack([jnp.concatenate(t, 1) for t in zip(*columns_of)])
        part = part.reshape(2, n_tp, rows, half)
        bit = 1
        while bit < n_tp:
            split = part.reshape(2, -1, 2, rows, half)
            which = (tp // bit) % 2
            keep = lax.dynamic_index_in_dim(split, which, 2, keepdims=False)
            send = lax.dynamic_index_in_dim(split, 1 - which, 2, keepdims=False)
            got = swap(send, "tp", bit, n_tp)
            part = (keep.astype(F32) + got.astype(F32)).astype(BF)
            bit *= 2
        mine = part.reshape(2, rows, half)[0]
        other = swap(part.reshape(2, rows, half)[1], "fs", 1, n_fs)
        both = jnp.where(
            y == 0, jnp.stack([mine, other], 1), jnp.stack([other, mine], 1)
        ).reshape(rows, 2, links, own)
        order = (c - jnp.arange(links)) % links
        grad_inputs = jnp.take(both, order, axis=2).transpose(0, 2, 1, 3)
        return (
            grad_inputs.reshape(rows, depth),
            grads[0],
            grads[1],
            jnp.sum(conv_gate * sums[0:3], axis=0),
            jnp.sum(conv_value * sums[3:6], axis=0),
            sums[0:3] * gate_scale,
            sums[3:6] * value_scale,
        )

    return on_device


def solution(mesh):
    placed = (
        P(("fs", "tp"), None),
        P("fs", "tp"),
        P("fs", "tp"),
        P("tp"),
        P("tp"),
        P(None, "tp"),
        P(None, "tp"),
        P("fs", "tp"),
        P("fs", "tp"),
        P("fs", "tp"),
    )
    body = make(mesh.shape["fs"], mesh.shape["tp"])

    return jax.shard_map(
        body,
        mesh=mesh,
        in_specs=placed,
        out_specs=(
            P(("fs", "tp"), None),
            P("fs", "tp"),
            P("fs", "tp"),
            P("tp"),
            P("tp"),
            P(None, "tp"),
            P(None, "tp"),
        ),
        check_vma=False,
    )
```

```python
import jax
import jax.numpy as jnp
from jax import lax
from jax.experimental import pallas as pl
from jax.experimental.pallas import tpu as pltpu
from jax.sharding import PartitionSpec as P


BF = jnp.bfloat16
F32 = jnp.float32


LANES = 128


def elementwise(gs_ref, vs_ref, cg_ref, cv_ref, g_ref, v_ref, up_ref, gc_ref, vc_ref, s_ref):
    tokens = g_ref.shape[0]
    row = lax.broadcasted_iota(jnp.int32, g_ref.shape, 0)

    def down(x, k):
        return jnp.where(row >= k, pltpu.roll(x, k, 0), 0.0)

    def up(x, k):
        return jnp.where(row < tokens - k, pltpu.roll(x, tokens - k, 0), 0.0)

    def shifted(ref):
        x = ref[...].astype(F32)
        return down(x, 2), down(x, 1), x

    def conv(taps, xs):
        return taps[0:1] * xs[0] + taps[1:2] * xs[1] + taps[2:3] * xs[2]

    def back(taps, d):
        return (taps[2:3] * d + taps[1:2] * up(d, 1) + taps[0:1] * up(d, 2)).astype(BF)

    gs, vs = shifted(g_ref), shifted(v_ref)
    g = conv(cg_ref[...] * gs_ref[...], gs)
    v = conv(cv_ref[...] * vs_ref[...], vs)
    sig = 1.0 / (1.0 + jnp.exp(-g))
    base = up_ref[...].astype(F32) * sig
    d_gate = base * v * (1.0 + g * (1.0 - sig))
    d_value = base * g
    for j in range(3):
        s_ref[j : j + 1] = jnp.sum(d_gate * gs[j], axis=0, keepdims=True)
        s_ref[3 + j : 4 + j] = jnp.sum(d_value * vs[j], axis=0, keepdims=True)
    s_ref[6:8] = jnp.zeros((2, g_ref.shape[1]), F32)
    gc_ref[...] = back(cg_ref[...], d_gate)
    vc_ref[...] = back(cv_ref[...], d_value)


def cotangents(gs, vs, cg, cv, g, v, up):
    tokens, columns = g.shape
    big = pl.BlockSpec((tokens, LANES), lambda i: (0, i))

    def small(n):
        return pl.BlockSpec((n, LANES), lambda i: (0, i))

    return pl.pallas_call(
        elementwise,
        grid=(pl.cdiv(columns, LANES),),
        in_specs=[small(1), small(1), small(3), small(3), big, big, big],
        out_specs=[big, big, small(8)],
        out_shape=[jax.ShapeDtypeStruct(g.shape, BF)] * 2
        + [jax.ShapeDtypeStruct((8, columns), F32)],
        compiler_params=pltpu.CompilerParams(vmem_limit_bytes=24 * 2**20),
        cost_estimate=pl.CostEstimate(
            flops=g.size * 400, bytes_accessed=g.size * 10, transcendentals=g.size
        ),
    )(gs[None], vs[None], cg, cv, g, v, up)


def rescale(gs_ref, vs_ref, g_ref, v_ref, out_ref):
    out_ref[0] = (g_ref[...] * gs_ref[...]).astype(BF)
    out_ref[1] = (v_ref[...] * vs_ref[...]).astype(BF)


def scaled_weights(gs, vs, g, v):
    own, columns = g.shape
    parts = 4
    block = pl.BlockSpec((own // parts, columns), lambda i: (i, 0))
    scale = pl.BlockSpec((1, columns), lambda i: (0, 0))
    return pl.pallas_call(
        rescale,
        grid=(parts,),
        in_specs=[scale, scale, block, block],
        out_specs=pl.BlockSpec((2, own // parts, columns), lambda i: (0, i, 0)),
        out_shape=jax.ShapeDtypeStruct((2, own, columns), BF),
        compiler_params=pltpu.CompilerParams(vmem_limit_bytes=24 * 2**20),
        cost_estimate=pl.CostEstimate(
            flops=g.size * 100, bytes_accessed=g.size * 12, transcendentals=0
        ),
    )(gs[None], vs[None], g, v)


def tdot(a, b):
    return lax.dot_general(a, b, (((0,), (0,)), ((), ())), preferred_element_type=F32)


def ndot(a, b):
    return lax.dot_general(a, b, (((1,), (1,)), ((), ())), preferred_element_type=F32)


def make(n_fs, n_tp):
    links = n_fs // 2

    def on_device(
        inputs,
        w_gate,
        w_value,
        gate_scale,
        value_scale,
        conv_gate,
        conv_value,
        gate_pre,
        value_pre,
        grad_out,
    ):
        fs = lax.axis_index("fs")
        tp = lax.axis_index("tp")
        c, y = fs // 2, fs % 2
        rows, depth = inputs.shape
        own = w_gate.shape[0]
        half = depth // 2
        tokens, columns = gate_pre.shape

        def swap(x, axis, bit, n):
            return lax.ppermute(x, axis, [(i, i ^ bit) for i in range(n)])

        def chain(x, right, senders):
            step = 1 if right else -1
            pairs = [(2 * s + j, 2 * (s + step) + j) for s in senders for j in (0, 1)]
            return lax.ppermute(x, "fs", pairs)

        stacked = scaled_weights(gate_scale, value_scale, w_gate, w_value)
        rights, lefts = [], []
        r = l = stacked
        for s in range(links - 1):
            r = chain(r, True, range(s, links - 1))
            l = chain(l, False, range(1, links - s))
            rights.append(r)
            lefts.append(l)

        by_half = inputs.reshape(rows, links, 2, own)
        mine = lax.dynamic_index_in_dim(by_half, y, 2, keepdims=False)
        other = lax.dynamic_index_in_dim(by_half, 1 - y, 2, keepdims=False)
        mine, other = mine.reshape(rows, half), other.reshape(rows, half)
        other = swap(other, "fs", 1, n_fs)
        x = jnp.stack([mine, other])[:, None]
        bit = n_tp // 2
        while bit:
            got = swap(x, "tp", bit, n_tp)
            high = (tp // bit) % 2 == 1
            x = jnp.where(high, jnp.stack([got, x], 2), jnp.stack([x, got], 2))
            x = x.reshape(2, -1, rows, half)
            bit //= 2
        x = x.reshape(2, tokens, half)

        gate_cot, value_cot, sums = cotangents(
            gate_scale, value_scale, conv_gate, conv_value, gate_pre, value_pre, grad_out
        )
        bit = n_fs // 2
        while bit:
            sums = sums + swap(sums, "fs", bit, n_fs)
            bit //= 2

        gate_theirs = swap(gate_cot, "fs", 1, n_fs)
        value_theirs = swap(value_cot, "fs", 1, n_fs)
        pair = [(gate_cot, gate_theirs), (value_cot, value_theirs)]

        def at(blocks, i):
            return lax.dynamic_index_in_dim(
                blocks, jnp.clip(i, 0, links - 1), 0, keepdims=False
            )

        def collect(parts):
            r = l = None
            for t in range(links - 1):
                send_r = at(parts, links - 1 - t + c)
                send_l = at(parts, c - (links - 1 - t) + 0)
                if t:
                    send_r = (send_r.astype(F32) + r.astype(F32)).astype(BF)
                    send_l = (send_l.astype(F32) + l.astype(F32)).astype(BF)
                r = chain(send_r, True, range(0, t + 1))
                l = chain(send_l, False, range(links - 1 - t, links))
            total = at(parts, c).astype(F32)
            if r is not None:
                total = total + r.astype(F32) + l.astype(F32)
            return total

        grads = []
        for (cot, theirs), scale in zip(pair, (gate_scale, value_scale)):
            first = tdot(x[0], cot)
            parts = (first + tdot(x[1], theirs)).astype(BF)
            blocks = parts.reshape(links, own, columns)
            grads.append(collect(blocks) * scale)

        blocks = [stacked]
        for s in range(links - 1):
            blocks.append(jnp.where(c > s, rights[s], lefts[links - 2 - s]))
        columns_of = []
        for block in blocks:
            columns_of.append(
                [
                    (ndot(g, block[0]) + ndot(v, block[1])).astype(BF)
                    for g, v in zip(pair[0], pair[1])
                ]
            )
        part = jnp.stack([jnp.concatenate(t, 1) for t in zip(*columns_of)])
        part = part.reshape(2, n_tp, rows, half)
        bit = 1
        while bit < n_tp:
            split = part.reshape(2, -1, 2, rows, half)
            which = (tp // bit) % 2
            keep = lax.dynamic_index_in_dim(split, which, 2, keepdims=False)
            send = lax.dynamic_index_in_dim(split, 1 - which, 2, keepdims=False)
            got = swap(send, "tp", bit, n_tp)
            part = (keep.astype(F32) + got.astype(F32)).astype(BF)
            bit *= 2
        mine = part.reshape(2, rows, half)[0]
        other = swap(part.reshape(2, rows, half)[1], "fs", 1, n_fs)
        both = jnp.where(
            y == 0, jnp.stack([mine, other], 1), jnp.stack([other, mine], 1)
        ).reshape(rows, 2, links, own)
        order = (c - jnp.arange(links)) % links
        grad_inputs = jnp.take(both, order, axis=2).transpose(0, 2, 1, 3)
        return (
            grad_inputs.reshape(rows, depth),
            grads[0],
            grads[1],
            jnp.sum(conv_gate * sums[0:3], axis=0),
            jnp.sum(conv_value * sums[3:6], axis=0),
            sums[0:3] * gate_scale,
            sums[3:6] * value_scale,
        )

    return on_device


def solution(mesh):
    placed = (
        P(("fs", "tp"), None),
        P("fs", "tp"),
        P("fs", "tp"),
        P("tp"),
        P("tp"),
        P(None, "tp"),
        P(None, "tp"),
        P("fs", "tp"),
        P("fs", "tp"),
        P("fs", "tp"),
    )
    body = make(mesh.shape["fs"], mesh.shape["tp"])

    return jax.shard_map(
        body,
        mesh=mesh,
        in_specs=placed,
        out_specs=(
            P(("fs", "tp"), None),
            P("fs", "tp"),
            P("fs", "tp"),
            P("tp"),
            P("tp"),
            P(None, "tp"),
            P(None, "tp"),
        ),
        check_vma=False,
    )
```
